32 devices in a mesh: sp: 4 (over y, x), tp: 8 (over z, core).
Axes of the slice: x: 2, y: 2, z: 4, core: 2. Of those that a mesh axis runs over, the one named last changes fastest.
Arguments:
- layer_input: bfloat16 [1024, 4096], P('sp', 'tp'), may hold values from -6 to 6
- out_cotangent: bfloat16 [1024, 4096], P('sp', 'tp'), may hold values from -1.5 to 1.5
- routes: int32 [1024, 2], P('sp'), may hold values from 0 to 3, all different within a row; in each aligned block of 256 rows (0 to 255, 256 to 511, ...) at most 160 rows name the same one
- route_weights: float32 [1024, 2], P('sp'), may hold values from 0.2 to 1
- gate_proj: bfloat16 [4, 4096, 2048], P('sp', None, 'tp'), may hold values from -0.09375 to 0.09375
- up_proj: bfloat16 [4, 4096, 2048], P('sp', None, 'tp'), may hold values from -0.09375 to 0.09375
- down_proj: bfloat16 [4, 2048, 4096], P('sp', 'tp'), may hold values from -0.125 to 0.125
- out_proj: bfloat16 [4096, 4096], P(None, 'tp'), may hold values from -0.09375 to 0.09375
- mixer_output: bfloat16 [1024, 4096], P('sp', 'tp'), may hold values from -0.29882812 to 0.29882812
- queries: bfloat16 [1024, 2048], P('sp', 'tp'), may hold values from -6 to 6
- key_rows: bfloat16 [1024, 2048], P('sp', 'tp'), may hold values from -6 to 6
- value_rows: bfloat16 [1024, 4096], P('sp', 'tp'), may hold values from -0.3984375 to 0.3984375
- log_decay: float32 [1024, 2048], P('sp', 'tp'), may hold values from -1.5 to 0, as said below
- entry_state: float32 [4, 16, 128, 256], P('sp', 'tp'), may hold values from -6 to 6
Outputs:
- gate_proj_grad: bfloat16 [4, 4096, 2048], P('sp', None, 'tp')
- up_proj_grad: bfloat16 [4, 4096, 2048], P('sp', None, 'tp')
- down_proj_grad: bfloat16 [4, 2048, 4096], P('sp', 'tp')
- out_proj_grad: float32 [4096, 4096], P('sp', 'tp')
- query_grad: bfloat16 [1024, 2048], P('sp', 'tp')
- key_grad: bfloat16 [1024, 2048], P('sp', 'tp')
- value_grad: bfloat16 [1024, 4096], P('sp', 'tp')
- decay_grad: float32 [1024, 2048], P('sp', 'tp')
The draws below stay inside these ranges and needn't reach their ends.
Inputs may be any that keep to these rules, and one draw needn't show every extreme that they name: `routes`: each token names 2 different experts. Among the tokens of one index of sp no expert is named more than 160 times, and in every draw some expert is named exactly 160 times by the tokens of some index of sp. `log_decay`: every entry is negative.
All inputs are finite; a program needn't handle non-finite values.
Results may differ from the reference program's by a relative error of at most 0.022.
Values may be sent and summed in bfloat16 or wider, within the bound.
No kernel may reach another device: no remote copies, remote signals or barrier semaphores. Data moves between devices by JAX's collectives and lax.ppermute only.
A program may use at most 128 MiB of HBM per device.

```python
import math
import jax
import jax.numpy as jnp
import numpy as np
from jax import lax

D = 4096
HEADS = 16
DK = 128
DV = 256
FF = 2048
TOP = 2
SPAN = 64
TOK_DEV = 256
EXPERTS = 4
TOKEN_COUNT = 1024
CAP = 160
N_SP = 4


def draw_log_decay(key, part):
    key_matrix = jax.random.split(jax.random.fold_in(key, 17), 7)
    channel_count = HEADS * DK
    fast_share = 0.5
    is_fast = jax.random.uniform(key_matrix[0], (channel_count,)) < fast_share
    slow_rate = jax.random.uniform(key_matrix[1], (channel_count,), minval=0.05, maxval=0.35) * (math.log(10.0) / TOKEN_COUNT)
    fast_rate = jax.random.uniform(key_matrix[2], (channel_count,), minval=1.0 / 100.0, maxval=1.0 / 30.0)
    rate = jnp.where(is_fast, fast_rate, slow_rate)
    device_blocks = TOKEN_COUNT // TOK_DEV
    device_factor = jnp.exp(jax.random.uniform(key_matrix[3], (device_blocks, 1, 1), minval=-0.7, maxval=0.7))
    rough = jax.random.uniform(key_matrix[4], (device_blocks, TOK_DEV, channel_count), minval=0.5, maxval=1.5)
    starting_offset = (rate[None, None, :] * device_factor * rough).reshape(TOKEN_COUNT, channel_count)
    group_position = jax.random.randint(key_matrix[5], (3,), 0, TOKEN_COUNT)
    group_length = jax.random.uniform(key_matrix[6], (3, channel_count), minval=0.22, maxval=0.4)
    position_index = jnp.arange(TOKEN_COUNT, dtype=jnp.int32)
    group_slot_hits = (position_index[:, None] == group_position[None, :]).astype(jnp.float32)
    token_groups = jnp.dot(group_slot_hits, group_length)
    return -(starting_offset + token_groups)


def strengthened(drawn, key, source, target, blocks, factor):
    def block_of(dim):
        return (jnp.arange(drawn.shape[dim]) // (drawn.shape[dim] // blocks)).reshape((-1,) + (1,) * (drawn.ndim - 1 - dim))

    one_side = jax.random.permutation(key, blocks)[block_of(target)]
    far = (block_of(target) + blocks // 2) % blocks
    return jnp.where((block_of(source) == one_side) | (block_of(source) == far), factor * drawn, drawn)


def level_of(key, shape, cuts, smallest, largest):
    gain, own = 1.0, jax.random.fold_in(key, 6)
    for axis_at, parts in cuts:
        heights = jnp.exp(jax.random.uniform(jax.random.fold_in(own, axis_at), (parts,), jnp.float32, smallest / len(cuts), largest / len(cuts)))
        gain = gain * jnp.repeat(heights, shape[axis_at] // parts).reshape([-1 if axis == axis_at else 1 for axis in range(len(shape))])
    return gain


def routed_block(rng, own, number, rows, count, top, limit, lean):
    ranking = jax.random.permutation(rng, count)
    packed, usual = load_shares(count, rows * top, limit, lean, True), load_shares(count, rows * top, limit, lean, False)
    places = jnp.arange(count)

    def named(lengths, turn):
        used = int((lengths > 0).sum())
        fixed = max(1, used // 4)
        moved = fixed + (places - fixed + turn * (used - fixed)) % max(1, count - fixed)
        return jnp.zeros((count,), jnp.int32).at[ranking[jnp.where(places < fixed, places, moved)]].set(jnp.asarray(lengths, jnp.int32))

    lengths = jnp.where(number % 4 == 0, named(packed, number // 4), named(usual, number - number // 4 - 1))
    mixed = jax.random.permutation(jax.random.fold_in(own, 3), count)
    giver, taker = mixed[0:count // 2 * 2:2], mixed[1:count // 2 * 2:2]
    slack = jnp.minimum(lengths[giver] - 1, limit - lengths[taker]) // 2
    slack = jnp.where((giver == ranking[0]) | (taker == ranking[0]) | (lengths[taker] == 0), 0, jnp.maximum(slack, 0))
    moved = jax.random.randint(jax.random.fold_in(own, 4), (count // 2,), 0, 1 << 20) % (slack + 1)
    lengths = lengths.at[giver].add(-moved).at[taker].add(moved)
    members = jnp.searchsorted(jnp.cumsum(lengths), jnp.arange(rows * top), side="right").astype(jnp.int32)
    listing = members.reshape(top, rows).T
    listing = listing[jax.random.permutation(jax.random.fold_in(own, 1), rows)]
    turn = jax.random.randint(jax.random.fold_in(own, 2), (rows, 1), 0, top)
    return jnp.take_along_axis(listing, (jnp.arange(top)[None, :] + turn) % top, axis=1)


def load_shares(amount, total, limit, lean, full):
    loads = [(1 << 20) // math.isqrt(rank ** lean) + 1 for rank in range(1, amount + 1)]
    largest = limit if full else min(limit, max(-(-total // amount), total * loads[0] // sum(loads)))
    least = 1 if total - largest >= amount - 1 else 0
    given, rest = [largest] + [least] * (amount - 1), total - largest - least * (amount - 1)
    while rest > 0:
        free = [i for i in range(1, amount) if given[i] < largest] or [i for i in range(1, amount) if given[i] < limit]
        whole, budget = sum([loads[i] for i in free]), rest
        for i in free:
            extra = min(limit - given[i], max(1, budget * loads[i] // whole), rest)
            given[i] = given[i] + extra
            rest = rest - extra
    return np.array(given)


def scatter_about(rng, extent, scale, limit, shards=(), kind=jnp.bfloat16):
    drawn = jax.random.normal(rng, extent, jnp.float32) * scale
    if len(shards) > 0:
        drawn = level_of(rng, extent, shards, -0.22, 0.18) * drawn
    return jnp.clip(drawn, min=-limit, max=limit).astype(kind)


def heavy_noise(stream_key, shape, scale, limit, shards, heavy, kind=jnp.bfloat16):
    result = scale * jax.random.normal(stream_key, shape, jnp.float32)
    if shards:
        result = result * level_of(stream_key, shape, shards, -0.22, 0.18)
    return jnp.clip(strengthened(result, jax.random.fold_in(stream_key, 3), *heavy), -limit, limit).astype(kind)


def setup_inputs(seed: int = 0) -> dict:
    splits = jax.random.split(jax.random.key(seed), 15)
    layer_input = scatter_about(splits[0], (TOKEN_COUNT, D), 1.0, 6.0, ((0, 4), (1, 8)))
    out_cotangent = heavy_noise(splits[1], (TOKEN_COUNT, D), 0.25, 1.5, ((0, 4), (1, 8)), (0, 1, 8, 2.0))
    routes_keys = jax.random.split(jax.random.fold_in(splits[2], 1), TOKEN_COUNT // TOK_DEV)
    routes_turns = jax.random.permutation(jax.random.fold_in(splits[2], 3), TOKEN_COUNT // TOK_DEV)
    routes = jax.vmap(lambda own, number: routed_block(jax.random.fold_in(splits[2], 2), own, number, TOK_DEV, EXPERTS, TOP, CAP, 0))(routes_keys, routes_turns).reshape((TOKEN_COUNT, TOP))
    route_weights = jnp.clip(0.2 + 0.8 * jax.random.uniform(splits[3], (TOKEN_COUNT, TOP), jnp.float32) ** level_of(splits[3], (TOKEN_COUNT, TOP), ((0, 4),), -0.2, 0.2), 0.2, 1.0)
    gate_proj = scatter_about(splits[4], (EXPERTS, D, FF), D ** -0.5, 0.09375, ((0, 4), (2, 8)))
    up_proj = scatter_about(splits[5], (EXPERTS, D, FF), D ** -0.5, 0.09375, ((0, 4), (2, 8)))
    down_proj = scatter_about(splits[6], (EXPERTS, FF, D), FF ** -0.5, 0.125, ((0, 4), (1, 8)))
    out_proj = scatter_about(splits[7], (D, HEADS * DV), (HEADS * DV) ** -0.5, 0.09375, ((1, 8),))
    mixer_output = scatter_about(splits[8], (TOKEN_COUNT, HEADS * DV), 0.05, 0.29882812, ((0, 4), (1, 8)))
    queries = scatter_about(splits[9], (TOKEN_COUNT, HEADS * DK), 1.0, 6.0, ((0, 4), (1, 8)))
    key_rows = scatter_about(splits[10], (TOKEN_COUNT, HEADS * DK), 1.0, 6.0, ((0, 4), (1, 8)))
    value_rows = scatter_about(splits[11], (TOKEN_COUNT, HEADS * DV), 0.0625, 0.3984375, ((0, 4), (1, 8)))
    log_decay = draw_log_decay(jax.random.fold_in(splits[14], 71), 0)
    entry_state = scatter_about(splits[13], (N_SP, HEADS, DK, DV), 1.0, 6.0, ((0, 4), (1, 8)), jnp.float32)
    return {"layer_input": layer_input, "out_cotangent": out_cotangent, "routes": routes, "route_weights": route_weights, "gate_proj": gate_proj, "up_proj": up_proj, "down_proj": down_proj, "out_proj": out_proj, "mixer_output": mixer_output, "queries": queries, "key_rows": key_rows, "value_rows": value_rows, "log_decay": log_decay, "entry_state": entry_state}


PRECISION_LEVEL = lax.Precision.HIGHEST


def expert_backward(inputs, pair_grad, gate_weight, up_weight, down_weight):
    gate_pre = jnp.dot(inputs, gate_weight, preferred_element_type=jnp.float32)
    up_pre = jnp.dot(inputs, up_weight, preferred_element_type=jnp.float32)
    sigmoid_gate = jax.nn.sigmoid(gate_pre)
    activated = gate_pre * sigmoid_gate
    hidden = (activated * up_pre).astype(jnp.bfloat16)
    down_grad = jnp.dot(hidden.T, pair_grad, preferred_element_type=jnp.float32)
    hidden_grad = jnp.dot(pair_grad, down_weight.T, preferred_element_type=jnp.float32)
    gate_delta = (hidden_grad * up_pre * sigmoid_gate * (1.0 + gate_pre * (1.0 - sigmoid_gate))).astype(jnp.bfloat16)
    up_delta = (hidden_grad * activated).astype(jnp.bfloat16)
    gate_grad = jnp.dot(inputs.T, gate_delta, preferred_element_type=jnp.float32)
    up_grad = jnp.dot(inputs.T, up_delta, preferred_element_type=jnp.float32)
    input_grad = jnp.dot(gate_delta, gate_weight.T, preferred_element_type=jnp.float32)
    input_grad = input_grad + jnp.dot(up_delta, up_weight.T, preferred_element_type=jnp.float32)
    return gate_grad.astype(jnp.bfloat16), up_grad.astype(jnp.bfloat16), down_grad.astype(jnp.bfloat16), input_grad


def slot_table(routes):
    blocks = routes.reshape(N_SP, TOK_DEV * TOP).astype(jnp.int32)
    expert_ids = jnp.arange(EXPERTS, dtype=jnp.int32)

    def block_rank(pair_ids):
        onehot = (pair_ids[:, None] == expert_ids[None, :]).astype(jnp.int32)
        return jnp.sum((jnp.cumsum(onehot, axis=0) - onehot) * onehot, axis=1)

    slot_rank = jax.vmap(block_rank)(blocks)
    source = jnp.arange(N_SP, dtype=jnp.int32)[:, None]
    row_pos = (source * CAP + slot_rank).astype(jnp.int32)
    pair_index = (source * (TOK_DEV * TOP) + jnp.arange(TOK_DEV * TOP, dtype=jnp.int32)[None, :]).astype(jnp.int32)
    table = jnp.full((EXPERTS, N_SP * CAP), TOKEN_COUNT * TOP, dtype=jnp.int32)
    return table.at[blocks, row_pos].set(pair_index)


def forward_block(passed_state, block_data):
    scaled_q, key_segment, value_segment, decays, output_gradient = block_data
    position_index = decays.shape[0]
    causal = jnp.tril(jnp.ones((position_index, position_index), dtype=bool))
    running_decay = jnp.cumsum(decays, axis=0)
    growth_multiplier = jnp.exp(running_decay)
    shrink = jnp.exp(-running_decay)
    block_overall_sum = running_decay[-1]
    value_dots = jnp.where(causal[None], jnp.einsum('thv,shv->hts', output_gradient, value_segment, precision=PRECISION_LEVEL), 0.0)
    state_contribution = growth_multiplier * jnp.einsum('gxb,xqb->gxq', output_gradient, passed_state, precision=PRECISION_LEVEL)
    inside = growth_multiplier * jnp.einsum('hts,shk->thk', value_dots, key_segment * shrink, precision=PRECISION_LEVEL)
    state_update = jnp.einsum('rsx,rse->sxe', key_segment * jnp.exp(block_overall_sum - running_decay), value_segment, precision=PRECISION_LEVEL)
    return jnp.exp(block_overall_sum)[:, :, None] * passed_state + state_update, state_contribution + inside


def reverse_block(passed_state, block_data):
    scaled_q, key_segment, value_segment, decays, output_gradient = block_data
    position_index = decays.shape[0]
    causal = jnp.tril(jnp.ones((position_index, position_index), dtype=bool))
    running_decay = jnp.cumsum(decays, axis=0)
    growth_multiplier = jnp.exp(running_decay)
    shrink = jnp.exp(-running_decay)
    block_overall_sum = running_decay[-1]
    decay_remaining = jnp.exp(block_overall_sum - running_decay)
    value_dots = jnp.where(causal[None], jnp.einsum('thv,shv->hts', output_gradient, value_segment, precision=PRECISION_LEVEL), 0.0)
    query_raised = scaled_q * growth_multiplier
    key_portion = decay_remaining * jnp.einsum('gxb,xqb->gxq', value_segment, passed_state, precision=PRECISION_LEVEL)
    key_portion = key_portion + shrink * jnp.einsum('hts,thk->shk', value_dots, query_raised, precision=PRECISION_LEVEL)
    scores = jnp.where(causal[None], jnp.einsum('thk,shk->hts', query_raised, key_segment * shrink, precision=PRECISION_LEVEL), 0.0)
    value_portion = jnp.einsum('qgy,gye->qge', key_segment * decay_remaining, passed_state, precision=PRECISION_LEVEL)
    value_portion = value_portion + jnp.einsum('hts,thv->shv', scores, output_gradient, precision=PRECISION_LEVEL)
    prior_steps = jnp.einsum('rsx,rse->sxe', query_raised, output_gradient, precision=PRECISION_LEVEL) + jnp.exp(block_overall_sum)[:, :, None] * passed_state
    return prior_steps, (key_portion, value_portion)


def mixer_backward(queries, key_rows, value_rows, log_decay, entry_state, mix_grad):
    blocks = TOK_DEV // SPAN

    def split(rows, width):
        return rows.astype(jnp.float32).reshape(N_SP, blocks, SPAN, HEADS, width)

    scaled_q = split(queries, DK) * (DK ** -0.5)
    key_segment = split(key_rows, DK)
    value_segment = split(value_rows, DV)
    decays = split(log_decay, DK)
    output_gradient = split(mix_grad, DV)

    def per_device(device_data):
        return lax.scan(forward_block, device_data[0], device_data[1:])[1]

    query_part = lax.map(per_device, (entry_state.astype(jnp.float32), scaled_q, key_segment, value_segment, decays, output_gradient))

    def joined(rows):
        return rows.reshape(N_SP * blocks, SPAN, HEADS, rows.shape[-1])

    start = jnp.zeros((HEADS, DK, DV), dtype=jnp.float32)
    sequence = (joined(scaled_q), joined(key_segment), joined(value_segment), joined(decays), joined(output_gradient))
    _, (key_portion, value_portion) = lax.scan(reverse_block, start, sequence, reverse=True)
    query_flat = query_part.reshape(TOKEN_COUNT, HEADS, DK)
    key_flattened = key_portion.reshape(TOKEN_COUNT, HEADS, DK)
    change = scaled_q.reshape(TOKEN_COUNT, HEADS, DK) * query_flat - key_segment.reshape(TOKEN_COUNT, HEADS, DK) * key_flattened
    decay_grad = lax.cumsum(change, axis=0, reverse=True).reshape(TOKEN_COUNT, HEADS * DK)
    query_grad = (query_flat * (DK ** -0.5)).reshape(TOKEN_COUNT, HEADS * DK).astype(jnp.bfloat16)
    key_grad = key_flattened.reshape(TOKEN_COUNT, HEADS * DK).astype(jnp.bfloat16)
    value_grad = value_portion.reshape(TOKEN_COUNT, HEADS * DV).astype(jnp.bfloat16)
    return query_grad, key_grad, value_grad, decay_grad


def reference(layer_input, out_cotangent, routes, route_weights, gate_proj, up_proj, down_proj, out_proj,
              mixer_output, queries, key_rows, value_rows, log_decay, entry_state):
    table = slot_table(routes)
    input_pad = jnp.concatenate([layer_input, jnp.zeros((1, D), dtype=layer_input.dtype)], axis=0)
    grad_pad = jnp.concatenate([out_cotangent.astype(jnp.float32), jnp.zeros((1, D), dtype=jnp.float32)], axis=0)
    weight_pad = jnp.concatenate([route_weights.reshape(-1).astype(jnp.float32), jnp.zeros((1,), dtype=jnp.float32)])

    def one_expert(expert_data):
        pair_ids, gate_weight, up_weight, down_weight = expert_data
        token_ids = (pair_ids // TOP).astype(jnp.int32)
        inputs = input_pad[token_ids]
        pair_grad = (weight_pad[pair_ids][:, None] * grad_pad[token_ids]).astype(jnp.bfloat16)
        return expert_backward(inputs, pair_grad, gate_weight, up_weight, down_weight)

    gate_proj_grad, up_proj_grad, down_proj_grad, row_grads = lax.map(one_expert, (table, gate_proj, up_proj, down_proj))
    token_ids = (table // TOP).astype(jnp.int32).reshape(-1)
    moe_grad = jnp.zeros((TOKEN_COUNT + 1, D), dtype=jnp.float32).at[token_ids].add(row_grads.reshape(-1, D))
    token_grad = (out_cotangent.astype(jnp.float32) + moe_grad[:TOKEN_COUNT]).astype(jnp.bfloat16)
    mix_grad = jnp.dot(token_grad, out_proj, preferred_element_type=jnp.float32).astype(jnp.bfloat16)
    out_proj_grad = jnp.dot(token_grad.T, mixer_output, preferred_element_type=jnp.float32)
    query_grad, key_grad, value_grad, decay_grad = mixer_backward(queries, key_rows, value_rows, log_decay, entry_state, mix_grad)
    return (gate_proj_grad, up_proj_grad, down_proj_grad, out_proj_grad, query_grad, key_grad, value_grad, decay_grad)
```

```python
import jax
import jax.numpy as jnp
from jax import lax
from jax.experimental import pallas as pl
from jax.experimental.pallas import tpu as pltpu
from jax.sharding import PartitionSpec as P

SPAN = 64
BF = jnp.bfloat16
F32 = jnp.float32
HI = lax.Precision.HIGHEST


def swapped(a, axis, distance):
    count = lax.axis_size(axis)
    return lax.ppermute(a, axis, [(i, i ^ distance) for i in range(count)])


def dot(a, b, dims):
    return lax.dot_general(a, b, (dims, ((), ())), preferred_element_type=F32)


def groups_of(count):
    groups, at = [[0]], 1
    while at < count:
        groups.append(list(range(at, 2 * at)))
        at *= 2
    return groups


def mixer_kernel(q_ref, k_ref, v_ref, g_ref, l_ref, s_ref, f_ref, dq_ref, dk_ref, dv_ref, da_ref):
    tokens = q_ref.shape[0]
    heads, dv, dk = s_ref.shape
    scale = dk ** (-0.5)
    row = lax.broadcasted_iota(jnp.int32, (SPAN, SPAN), 0)
    col = lax.broadcasted_iota(jnp.int32, (SPAN, SPAN), 1)
    causal = row >= col
    upper = (col >= row).astype(F32)
    for h in range(heads):
        ks = slice(h * dk, (h + 1) * dk)
        vs = slice(h * dv, (h + 1) * dv)
        state = s_ref[h]
        parts = []
        for n in range(tokens // SPAN):
            rows = slice(n * SPAN, (n + 1) * SPAN)
            q = q_ref[rows, ks].astype(F32) * scale
            k = k_ref[rows, ks].astype(F32)
            v = v_ref[rows, vs]
            g = g_ref[rows, vs]
            run = l_ref[rows, ks]
            total = run[SPAN - 1 : SPAN, :]
            grow = jnp.exp(run)
            remain = jnp.exp(total - run)
            up = jnp.exp(run - 0.5 * total)
            down = jnp.exp(0.5 * total - run)
            k_end = (k * remain).astype(BF)
            q_start = (q * grow).astype(BF)
            q_mid = (q * up).astype(BF)
            k_mid = (k * down).astype(BF)
            dots = jnp.where(causal, dot(g, v, ((1,), (1,))), 0.0).astype(BF)
            scores = jnp.where(causal, dot(q_mid, k_mid, ((1,), (1,))), 0.0).astype(BF)
            dq = grow * dot(g, state.astype(BF), ((1,), (0,))) + up * dot(dots, k_mid, ((1,), (0,)))
            keep = jnp.exp(total)
            state = keep * state + dot(v, k_end, ((0,), (0,)))
            dq_ref[rows, ks] = (dq * scale).astype(BF)
            parts.append((q, k, v, g, keep, remain, down, k_end, q_start, q_mid, dots, scores, dq))
        back = f_ref[h]
        carry = jnp.zeros((1, dk), F32)
        for n in reversed(range(tokens // SPAN)):
            rows = slice(n * SPAN, (n + 1) * SPAN)
            q, k, v, g, keep, remain, down, k_end, q_start, q_mid, dots, scores, dq = parts[n]
            back_b = back.astype(BF)
            dkey = remain * dot(v, back_b, ((1,), (0,))) + down * dot(dots, q_mid, ((0,), (0,)))
            dval = dot(k_end, back_b, ((1,), (1,))) + dot(scores, g, ((0,), (0,)))
            back = keep * back + dot(g, q_start, ((0,), (0,)))
            dk_ref[rows, ks] = dkey.astype(BF)
            dv_ref[rows, vs] = dval.astype(BF)
            change = q * dq - k * dkey
            sums = carry + lax.dot_general(
                upper, change, (((1,), (0,)), ((), ())), precision=HI, preferred_element_type=F32
            )
            da_ref[rows, ks] = sums
            carry = sums[0:1, :]


def body(
    layer_input,
    out_cotangent,
    routes,
    route_weights,
    gate_proj,
    up_proj,
    down_proj,
    out_proj,
    mixer_output,
    queries,
    key_rows,
    value_rows,
    log_decay,
    entry_state,
):
    nsp = lax.axis_size("sp")
    ntp = lax.axis_size("tp")
    nz = ntp // 2
    my_sp = lax.axis_index("sp")
    my_tp = lax.axis_index("tp")
    local = gate_proj.shape[0]
    experts = local * nsp
    tokens, cols = layer_input.shape
    top = routes.shape[1]
    cap = 5 * top * tokens // (4 * experts)
    per = local * cap
    groups = groups_of(nz)

    order = [2 * d + h for h in range(2) for d in range(nz)]

    def to_relative(a, axis):
        size = a.shape[axis] // ntp
        return jnp.concatenate(
            [lax.dynamic_slice_in_dim(a, (k ^ my_tp) * size, size, axis) for k in order], axis
        )

    def place_of(shard):
        k = shard ^ my_tp
        return (k % 2) * nz + k // 2

    def to_absolute(a, axis):
        size = a.shape[axis] // ntp
        return jnp.concatenate(
            [lax.dynamic_slice_in_dim(a, place_of(p) * size, size, axis) for p in range(ntp)], axis
        )

    expert_ids = jnp.arange(experts, dtype=jnp.int32)
    named = routes[:, :, None] == expert_ids[None, None, :]
    members = jnp.any(named, axis=1).astype(BF)
    earlier = jnp.tril(jnp.ones((tokens, tokens), BF), -1)
    ranks = jnp.dot(earlier, members, preferred_element_type=F32)
    rank = jnp.sum(jnp.where(named, ranks[:, None, :], 0.0), axis=2).astype(jnp.int32)
    target = ((routes // local) ^ my_sp) * per + (routes % local) * cap + rank
    slot_ids = jnp.arange(nsp * per, dtype=jnp.int32)
    hits = target[:, :, None] == slot_ids[None, None, :]
    placed = jnp.any(hits, axis=1).astype(BF)
    slot_weight = jnp.sum(jnp.where(hits, route_weights[:, :, None], 0.0), axis=(0, 1))

    def dispatch(a, weight):
        pieces = [a] + [swapped(a, "tp", 2 * d) for d in range(1, nz)]
        halves = []
        for group in groups:
            piece = jnp.concatenate([pieces[d] for d in group], axis=1)
            slots = dot(placed, piece, ((0,), (0,)))
            if weight is not None:
                slots = slots * weight[:, None]
            slots = slots.astype(BF).reshape(nsp, local, cap, piece.shape[1])
            arrived = [slots[0]] + [swapped(slots[x], "sp", x) for x in range(1, nsp)]
            halves.append(jnp.concatenate(arrived, axis=1))
        others = [swapped(half, "tp", 1) for half in halves]
        return halves + others

    inputs = dispatch(layer_input, None)
    grads = dispatch(out_cotangent, slot_weight)

    gate_rel = to_relative(gate_proj, 1)
    up_rel = to_relative(up_proj, 1)
    down_rel = to_relative(down_proj, 2)
    out_rel = to_relative(out_proj, 0)

    def bounds():
        at = []
        for h in range(2):
            for group in groups:
                start = (h * nz + group[0]) * cols
                at.append((start, start + len(group) * cols))
        return at

    def over_pieces(pieces, term):
        total = None
        for piece, (lo, hi) in zip(pieces, bounds()):
            part = term(piece, lo, hi)
            total = part if total is None else total + part
        return total

    gate_pre = over_pieces(
        inputs,
        lambda a, lo, hi: jnp.einsum(
            "erd,edf->erf", a, gate_rel[:, lo:hi], preferred_element_type=F32
        ),
    )
    up_pre = over_pieces(
        inputs,
        lambda a, lo, hi: jnp.einsum(
            "erd,edf->erf", a, up_rel[:, lo:hi], preferred_element_type=F32
        ),
    )
    hidden_grad = over_pieces(
        grads,
        lambda a, lo, hi: jnp.einsum(
            "erd,efd->erf", a, down_rel[:, :, lo:hi], preferred_element_type=F32
        ),
    )
    sigmoid_gate = jax.nn.sigmoid(gate_pre)
    activated = gate_pre * sigmoid_gate
    hidden = (activated * up_pre).astype(BF)
    gate_delta = (
        hidden_grad * up_pre * sigmoid_gate * (1.0 + gate_pre * (1.0 - sigmoid_gate))
    ).astype(BF)
    up_delta = (hidden_grad * activated).astype(BF)

    def row_grads(lo, hi):
        return jnp.einsum(
            "erf,edf->erd", gate_delta, gate_rel[:, lo:hi], preferred_element_type=F32
        ) + jnp.einsum("erf,edf->erd", up_delta, up_rel[:, lo:hi], preferred_element_type=F32)

    at = bounds()
    count = len(groups)
    theirs = {}
    for n in reversed(range(count)):
        theirs[n] = swapped(row_grads(*at[count + n]).astype(BF), "tp", 1)
    moe = None
    received = []
    for n in reversed(range(count)):
        rows = (row_grads(*at[n]) + theirs[n].astype(F32)).astype(BF)
        width = rows.shape[2]
        rows = rows.reshape(local, nsp, cap, width)
        back = [rows[:, 0]] + [swapped(rows[:, x], "sp", x) for x in range(1, nsp)]
        slots = jnp.concatenate(back, axis=0).reshape(nsp * per, width)
        sums = dot(placed, slots, ((1,), (0,)))
        if n == 0:
            moe = sums
        else:
            sums = sums.astype(BF)
            for m, d in enumerate(groups[n]):
                received.append(swapped(sums[:, m * cols : (m + 1) * cols], "tp", 2 * d))
    token_grad = out_cotangent.astype(F32) + moe
    for piece in received:
        token_grad = token_grad + piece.astype(F32)
    token_grad = token_grad.astype(BF)

    own = [token_grad] + [swapped(token_grad, "tp", 2 * d) for d in range(1, nz)]
    token_pieces = []
    for group in groups:
        token_pieces.append(jnp.concatenate([own[d] for d in group], axis=1))
    token_pieces = token_pieces + [swapped(piece, "tp", 1) for piece in token_pieces]
    mix_grad = over_pieces(
        token_pieces, lambda a, lo, hi: dot(a, out_rel[lo:hi], ((1,), (0,)))
    ).astype(BF)

    heads, key_width, value_width = entry_state.shape[1:]
    position = jnp.arange(tokens)
    same = (position[:, None] // SPAN == position[None, :] // SPAN) & (
        position[:, None] >= position[None, :]
    )
    run = jnp.dot(same.astype(F32), log_decay, precision=HI)
    ends = run[SPAN - 1 :: SPAN]
    before = jnp.cumsum(ends, axis=0) - ends
    whole_run = run + jnp.repeat(before, SPAN, axis=0)
    total = jnp.sum(ends, axis=0)
    totals = [total] + [swapped(total, "sp", x) for x in range(1, nsp)]
    entry_t = jnp.swapaxes(entry_state[0], 1, 2)

    def by_head(a, width):
        return a.reshape(tokens, heads, width)

    q_start = (queries.astype(F32) * key_width ** (-0.5) * jnp.exp(whole_run)).astype(BF)
    k_end = (key_rows.astype(F32) * jnp.exp(total - whole_run)).astype(BF)
    carried = jnp.einsum(
        "thv,thk->hvk",
        by_head(value_rows, value_width),
        by_head(k_end, key_width),
        preferred_element_type=F32,
    )
    start = jnp.einsum(
        "thv,thk->hvk",
        by_head(mix_grad, value_width),
        by_head(q_start, key_width),
        preferred_element_type=F32,
    )
    sent = start.astype(BF)
    following = jnp.zeros_like(start)
    for x in range(1, nsp):
        source = my_sp ^ x
        between = jnp.zeros_like(total)
        for y in range(1, nsp):
            middle = my_sp ^ y
            between = between + jnp.where((middle > my_sp) & (middle < source), totals[y], 0.0)
        weight = jnp.where(source > my_sp, jnp.exp(between), 0.0).reshape(heads, 1, key_width)
        following = following + weight * swapped(sent, "sp", x).astype(F32)
    change_sum = jnp.sum(start * entry_t - carried * following, axis=1).reshape(-1)
    later = jnp.zeros_like(change_sum)
    for x in range(1, nsp):
        later = later + jnp.where((my_sp ^ x) > my_sp, swapped(change_sum, "sp", x), 0.0)
    query_grad, key_grad, value_grad, decay_local = pl.pallas_call(
        mixer_kernel,
        out_shape=(
            jax.ShapeDtypeStruct(queries.shape, BF),
            jax.ShapeDtypeStruct(key_rows.shape, BF),
            jax.ShapeDtypeStruct(value_rows.shape, BF),
            jax.ShapeDtypeStruct(log_decay.shape, F32),
        ),
        name="mixer",
    )(queries, key_rows, value_rows, mix_grad, run, entry_t, following)
    decay_grad = decay_local + later[None]

    full_rel = jnp.concatenate(token_pieces, axis=1)
    shards = ntp // nsp
    half = tokens // 2
    my_core = my_tp % 2

    def block_for(owner, a):
        return jnp.concatenate(
            [
                lax.dynamic_slice_in_dim(a, place_of(owner * shards + m) * cols, cols, 1)
                for m in range(shards)
            ],
            axis=1,
        )

    mine = lax.dynamic_slice_in_dim(full_rel, my_core * half, half, 0)
    sides = [swapped(block_for(my_sp ^ x, mine), "sp", x) for x in range(1, nsp)]
    near = jnp.concatenate(sides, axis=0)
    far = swapped(near, "tp", 1)
    mixer_late, _ = lax.optimization_barrier((mixer_output, token_grad))
    mixers = [swapped(mixer_late, "sp", x) for x in range(1, nsp)]
    mixer_rest = jnp.stack(mixers).reshape(nsp - 1, 2, half, mixer_output.shape[1])
    mixer_near = lax.dynamic_index_in_dim(mixer_rest, my_core, 1, False).reshape(-1, mixer_output.shape[1])
    mixer_far = lax.dynamic_index_in_dim(mixer_rest, 1 - my_core, 1, False).reshape(-1, mixer_output.shape[1])
    proj_grad = (
        dot(block_for(my_sp, full_rel), mixer_output, ((0,), (0,)))
        + dot(near, mixer_near, ((0,), (0,)))
        + dot(far, mixer_far, ((0,), (0,)))
    )

    all_inputs = jnp.concatenate(inputs, axis=2)
    all_grads = jnp.concatenate(grads, axis=2)
    gate_part = jnp.einsum(
        "erd,erf->edf", all_inputs, gate_delta, preferred_element_type=F32
    ).astype(BF)
    up_part = jnp.einsum("erd,erf->edf", all_inputs, up_delta, preferred_element_type=F32).astype(BF)
    down_part = jnp.einsum("erf,erd->efd", hidden, all_grads, preferred_element_type=F32).astype(BF)
    return (
        to_absolute(gate_part, 1),
        to_absolute(up_part, 1),
        to_absolute(down_part, 2),
        proj_grad,
        query_grad,
        key_grad,
        value_grad,
        decay_grad,
    )


def solution(mesh):
    return jax.shard_map(
        body,
        mesh=mesh,
        in_specs=(
            P("sp", "tp"),
            P("sp", "tp"),
            P("sp", None),
            P("sp", None),
            P("sp", None, "tp"),
            P("sp", None, "tp"),
            P("sp", "tp", None),
            P(None, "tp"),
            P("sp", "tp"),
            P("sp", "tp"),
            P("sp", "tp"),
            P("sp", "tp"),
            P("sp", "tp"),
            P("sp", "tp", None, None),
        ),
        out_specs=(
            P("sp", None, "tp"),
            P("sp", None, "tp"),
            P("sp", "tp", None),
            P("sp", "tp"),
            P("sp", "tp"),
            P("sp", "tp"),
            P("sp", "tp"),
            P("sp", "tp"),
        ),
        check_vma=False,
    )
```

```python
import jax
import jax.numpy as jnp
from jax import lax
from jax.experimental import pallas as pl
from jax.experimental.pallas import tpu as pltpu
from jax.sharding import PartitionSpec as P

SPAN = 64
BF = jnp.bfloat16
F32 = jnp.float32
HI = lax.Precision.HIGHEST


def swapped(a, axis, distance):
    count = lax.axis_size(axis)
    return lax.ppermute(a, axis, [(i, i ^ distance) for i in range(count)])


def dot(a, b, dims):
    return lax.dot_general(a, b, (dims, ((), ())), preferred_element_type=F32)


def groups_of(count):
    groups, at = [[0]], 1
    while at < count:
        groups.append(list(range(at, 2 * at)))
        at *= 2
    return groups


def mixer_kernel(q_ref, k_ref, v_ref, g_ref, l_ref, s_ref, f_ref, dq_ref, dk_ref, dv_ref, da_ref):
    tokens = q_ref.shape[0]
    heads, dv, dk = s_ref.shape
    scale = dk ** (-0.5)
    row = lax.broadcasted_iota(jnp.int32, (SPAN, SPAN), 0)
    col = lax.broadcasted_iota(jnp.int32, (SPAN, SPAN), 1)
    causal = row >= col
    upper = (col >= row).astype(F32)
    for h in range(heads):
        ks = slice(h * dk, (h + 1) * dk)
        vs = slice(h * dv, (h + 1) * dv)
        state = s_ref[h]
        parts = []
        for n in range(tokens // SPAN):
            rows = slice(n * SPAN, (n + 1) * SPAN)
            q = q_ref[rows, ks].astype(F32) * scale
            k = k_ref[rows, ks].astype(F32)
            v = v_ref[rows, vs]
            g = g_ref[rows, vs]
            run = l_ref[rows, ks]
            total = run[SPAN - 1 : SPAN, :]
            grow = jnp.exp(run)
            remain = jnp.exp(total - run)
            up = jnp.exp(run - 0.5 * total)
            down = jnp.exp(0.5 * total - run)
            k_end = (k * remain).astype(BF)
            q_start = (q * grow).astype(BF)
            q_mid = (q * up).astype(BF)
            k_mid = (k * down).astype(BF)
            dots = jnp.where(causal, dot(g, v, ((1,), (1,))), 0.0).astype(BF)
            scores = jnp.where(causal, dot(q_mid, k_mid, ((1,), (1,))), 0.0).astype(BF)
            dq = grow * dot(g, state.astype(BF), ((1,), (0,))) + up * dot(dots, k_mid, ((1,), (0,)))
            keep = jnp.exp(total)
            state = keep * state + dot(v, k_end, ((0,), (0,)))
            dq_ref[rows, ks] = (dq * scale).astype(BF)
            parts.append((q, k, v, g, keep, remain, down, k_end, q_start, q_mid, dots, scores, dq))
        back = f_ref[h]
        carry = jnp.zeros((1, dk), F32)
        for n in reversed(range(tokens // SPAN)):
            rows = slice(n * SPAN, (n + 1) * SPAN)
            q, k, v, g, keep, remain, down, k_end, q_start, q_mid, dots, scores, dq = parts[n]
            back_b = back.astype(BF)
            dkey = remain * dot(v, back_b, ((1,), (0,))) + down * dot(dots, q_mid, ((0,), (0,)))
            dval = dot(k_end, back_b, ((1,), (1,))) + dot(scores, g, ((0,), (0,)))
            back = keep * back + dot(g, q_start, ((0,), (0,)))
            dk_ref[rows, ks] = dkey.astype(BF)
            dv_ref[rows, vs] = dval.astype(BF)
            change = q * dq - k * dkey
            sums = carry + lax.dot_general(
                upper, change, (((1,), (0,)), ((), ())), precision=HI, preferred_element_type=F32
            )
            da_ref[rows, ks] = sums
            carry = sums[0:1, :]


def body(
    layer_input,
    out_cotangent,
    routes,
    route_weights,
    gate_proj,
    up_proj,
    down_proj,
    out_proj,
    mixer_output,
    queries,
    key_rows,
    value_rows,
    log_decay,
    entry_state,
):
    nsp = lax.axis_size("sp")
    ntp = lax.axis_size("tp")
    nz = ntp // 2
    my_sp = lax.axis_index("sp")
    my_tp = lax.axis_index("tp")
    local = gate_proj.shape[0]
    experts = local * nsp
    tokens, cols = layer_input.shape
    top = routes.shape[1]
    cap = 5 * top * tokens // (4 * experts)
    per = local * cap
    groups = groups_of(nz)

    order = [2 * d + h for h in range(2) for d in range(nz)]

    def to_relative(a, axis, offset):
        size = a.shape[axis] // ntp
        return jnp.concatenate(
            [lax.dynamic_slice_in_dim(a, (k ^ my_tp) * size + offset, size, axis) for k in order],
            axis,
        )

    def place_of(shard):
        k = shard ^ my_tp
        return (k % 2) * nz + k // 2

    def to_absolute(a, axis):
        size = a.shape[axis] // ntp
        return jnp.concatenate(
            [lax.dynamic_slice_in_dim(a, place_of(p) * size, size, axis) for p in range(ntp)], axis
        )

    expert_ids = jnp.arange(experts, dtype=jnp.int32)
    named = routes[:, :, None] == expert_ids[None, None, :]
    members = jnp.any(named, axis=1).astype(BF)
    earlier = jnp.tril(jnp.ones((tokens, tokens), BF), -1)
    ranks = jnp.dot(earlier, members, preferred_element_type=F32)
    rank = jnp.sum(jnp.where(named, ranks[:, None, :], 0.0), axis=2).astype(jnp.int32)
    target = ((routes // local) ^ my_sp) * per + (routes % local) * cap + rank
    slot_ids = jnp.arange(nsp * per, dtype=jnp.int32)
    hits = target[:, :, None] == slot_ids[None, None, :]
    placed = jnp.any(hits, axis=1).astype(BF)
    slot_weight = jnp.sum(jnp.where(hits, route_weights[:, :, None], 0.0), axis=(0, 1))

    def dispatch(a, weight):
        pieces = [a] + [swapped(a, "tp", 2 * d) for d in range(1, nz)]
        halves = []
        for group in groups:
            piece = jnp.concatenate([pieces[d] for d in group], axis=1)
            slots = dot(placed, piece, ((0,), (0,)))
            if weight is not None:
                slots = slots * weight[:, None]
            slots = slots.astype(BF).reshape(nsp, local, cap, piece.shape[1])
            arrived = [slots[0]] + [swapped(slots[x], "sp", x) for x in range(1, nsp)]
            halves.append(jnp.concatenate(arrived, axis=1))
        others = [swapped(half, "tp", 1) for half in halves]
        return halves + others, slots

    inputs, _ = dispatch(layer_input, None)
    grads, last_slots = dispatch(out_cotangent, slot_weight)

    corner = last_slots[0, 0, 0, 0].astype(F32)
    zero = jnp.minimum(jnp.abs(corner), 0.0).astype(jnp.int32)

    gate_rel = to_relative(gate_proj, 1, zero)
    up_rel = to_relative(up_proj, 1, zero)
    down_rel = to_relative(down_proj, 2, zero)
    out_rel = to_relative(out_proj, 0, zero)

    def bounds():
        at = []
        for h in range(2):
            for group in groups:
                start = (h * nz + group[0]) * cols
                at.append((start, start + len(group) * cols))
        return at

    def over_pieces(pieces, term):
        total = None
        for piece, (lo, hi) in zip(pieces, bounds()):
            part = term(piece, lo, hi)
            total = part if total is None else total + part
        return total

    gate_pre = over_pieces(
        inputs,
        lambda a, lo, hi: jnp.einsum(
            "erd,edf->erf", a, gate_rel[:, lo:hi], preferred_element_type=F32
        ),
    )
    up_pre = over_pieces(
        inputs,
        lambda a, lo, hi: jnp.einsum(
            "erd,edf->erf", a, up_rel[:, lo:hi], preferred_element_type=F32
        ),
    )
    hidden_grad = over_pieces(
        grads,
        lambda a, lo, hi: jnp.einsum(
            "erd,efd->erf", a, down_rel[:, :, lo:hi], preferred_element_type=F32
        ),
    )
    sigmoid_gate = jax.nn.sigmoid(gate_pre)
    activated = gate_pre * sigmoid_gate
    hidden = (activated * up_pre).astype(BF)
    gate_delta = (
        hidden_grad * up_pre * sigmoid_gate * (1.0 + gate_pre * (1.0 - sigmoid_gate))
    ).astype(BF)
    up_delta = (hidden_grad * activated).astype(BF)

    def row_grads(lo, hi):
        return jnp.einsum(
            "erf,edf->erd", gate_delta, gate_rel[:, lo:hi], preferred_element_type=F32
        ) + jnp.einsum("erf,edf->erd", up_delta, up_rel[:, lo:hi], preferred_element_type=F32)

    at = bounds()
    count = len(groups)
    theirs = {}
    for n in reversed(range(count)):
        theirs[n] = swapped(row_grads(*at[count + n]).astype(BF), "tp", 1)
    moe = None
    received = []
    last_rows = []
    for n in reversed(range(count)):
        rows = (row_grads(*at[n]) + theirs[n].astype(F32)).astype(BF)
        width = rows.shape[2]
        rows = rows.reshape(local, nsp, cap, width)
        last_rows.append(rows)
        back = [rows[:, 0]] + [swapped(rows[:, x], "sp", x) for x in range(1, nsp)]
        slots = jnp.concatenate(back, axis=0).reshape(nsp * per, width)
        sums = dot(placed, slots, ((1,), (0,)))
        if n == 0:
            moe = sums
        else:
            sums = sums.astype(BF)
            for m, d in enumerate(groups[n]):
                received.append(swapped(sums[:, m * cols : (m + 1) * cols], "tp", 2 * d))
    token_grad = out_cotangent.astype(F32) + moe
    for piece in received:
        token_grad = token_grad + piece.astype(F32)
    token_grad = token_grad.astype(BF)

    own = [token_grad] + [swapped(token_grad, "tp", 2 * d) for d in range(1, nz)]
    token_pieces = []
    for group in groups:
        token_pieces.append(jnp.concatenate([own[d] for d in group], axis=1))
    token_pieces = token_pieces + [swapped(piece, "tp", 1) for piece in token_pieces]
    mix_grad = over_pieces(
        token_pieces, lambda a, lo, hi: dot(a, out_rel[lo:hi], ((1,), (0,)))
    ).astype(BF)

    heads, key_width, value_width = entry_state.shape[1:]
    position = jnp.arange(tokens)
    same = (position[:, None] // SPAN == position[None, :] // SPAN) & (
        position[:, None] >= position[None, :]
    )
    run = jnp.dot(same.astype(F32), log_decay, precision=HI)
    ends = run[SPAN - 1 :: SPAN]
    before = jnp.cumsum(ends, axis=0) - ends
    whole_run = run + jnp.repeat(before, SPAN, axis=0)
    total = jnp.sum(ends, axis=0)
    totals = [total] + [swapped(total, "sp", x) for x in range(1, nsp)]
    entry_t = jnp.swapaxes(entry_state[0], 1, 2)

    def by_head(a, width):
        return a.reshape(tokens, heads, width)

    q_start = (queries.astype(F32) * key_width ** (-0.5) * jnp.exp(whole_run)).astype(BF)
    k_end = (key_rows.astype(F32) * jnp.exp(total - whole_run)).astype(BF)
    carried = jnp.einsum(
        "thv,thk->hvk",
        by_head(value_rows, value_width),
        by_head(k_end, key_width),
        preferred_element_type=F32,
    )
    start = jnp.einsum(
        "thv,thk->hvk",
        by_head(mix_grad, value_width),
        by_head(q_start, key_width),
        preferred_element_type=F32,
    )
    sent = start.astype(BF)
    following = jnp.zeros_like(start)
    for x in range(1, nsp):
        source = my_sp ^ x
        between = jnp.zeros_like(total)
        for y in range(1, nsp):
            middle = my_sp ^ y
            between = between + jnp.where((middle > my_sp) & (middle < source), totals[y], 0.0)
        weight = jnp.where(source > my_sp, jnp.exp(between), 0.0).reshape(heads, 1, key_width)
        following = following + weight * swapped(sent, "sp", x).astype(F32)
    change_sum = jnp.sum(start * entry_t - carried * following, axis=1).reshape(-1)
    later = jnp.zeros_like(change_sum)
    for x in range(1, nsp):
        later = later + jnp.where((my_sp ^ x) > my_sp, swapped(change_sum, "sp", x), 0.0)
    query_grad, key_grad, value_grad, decay_local = pl.pallas_call(
        mixer_kernel,
        out_shape=(
            jax.ShapeDtypeStruct(queries.shape, BF),
            jax.ShapeDtypeStruct(key_rows.shape, BF),
            jax.ShapeDtypeStruct(value_rows.shape, BF),
            jax.ShapeDtypeStruct(log_decay.shape, F32),
        ),
        name="mixer",
    )(queries, key_rows, value_rows, mix_grad, run, entry_t, following)
    decay_grad = decay_local + later[None]

    full_rel = jnp.concatenate(token_pieces, axis=1)
    shards = ntp // nsp
    half = tokens // 2
    my_core = my_tp % 2

    def block_for(owner, a):
        return jnp.concatenate(
            [
                lax.dynamic_slice_in_dim(a, place_of(owner * shards + m) * cols, cols, 1)
                for m in range(shards)
            ],
            axis=1,
        )

    mine = lax.dynamic_slice_in_dim(full_rel, my_core * half, half, 0)
    sides = [swapped(block_for(my_sp ^ x, mine), "sp", x) for x in range(1, nsp)]
    near = jnp.concatenate(sides, axis=0)
    far = swapped(near, "tp", 1)
    mixer_late, _ = lax.optimization_barrier((mixer_output, token_grad))
    mixers = [swapped(mixer_late, "sp", x) for x in range(1, nsp)]
    mixer_rest = jnp.stack(mixers).reshape(nsp - 1, 2, half, mixer_output.shape[1])
    mixer_near = lax.dynamic_index_in_dim(mixer_rest, my_core, 1, False).reshape(-1, mixer_output.shape[1])
    mixer_far = lax.dynamic_index_in_dim(mixer_rest, 1 - my_core, 1, False).reshape(-1, mixer_output.shape[1])
    proj_grad = (
        dot(block_for(my_sp, full_rel), mixer_output, ((0,), (0,)))
        + dot(near, mixer_near, ((0,), (0,)))
        + dot(far, mixer_far, ((0,), (0,)))
    )

    nil = sum(jnp.minimum(jnp.abs(rows[0, 0, 0, 0].astype(F32)), 0.0) for rows in last_rows)
    gate_delta = (gate_delta.astype(F32) + nil).astype(BF)
    up_delta = (up_delta.astype(F32) + nil).astype(BF)
    hidden = (hidden.astype(F32) + nil).astype(BF)
    all_inputs = jnp.concatenate(inputs, axis=2)
    all_grads = jnp.concatenate(grads, axis=2)
    gate_part = jnp.einsum(
        "erd,erf->edf", all_inputs, gate_delta, preferred_element_type=F32
    ).astype(BF)
    up_part = jnp.einsum("erd,erf->edf", all_inputs, up_delta, preferred_element_type=F32).astype(BF)
    down_part = jnp.einsum("erf,erd->efd", hidden, all_grads, preferred_element_type=F32).astype(BF)
    return (
        to_absolute(gate_part, 1),
        to_absolute(up_part, 1),
        to_absolute(down_part, 2),
        proj_grad,
        query_grad,
        key_grad,
        value_grad,
        decay_grad,
    )


def solution(mesh):
    return jax.shard_map(
        body,
        mesh=mesh,
        in_specs=(
            P("sp", "tp"),
            P("sp", "tp"),
            P("sp", None),
            P("sp", None),
            P("sp", None, "tp"),
            P("sp", None, "tp"),
            P("sp", "tp", None),
            P(None, "tp"),
            P("sp", "tp"),
            P("sp", "tp"),
            P("sp", "tp"),
            P("sp", "tp"),
            P("sp", "tp"),
            P("sp", "tp", None, None),
        ),
        out_specs=(
            P("sp", None, "tp"),
            P("sp", None, "tp"),
            P("sp", "tp", None),
            P("sp", "tp"),
            P("sp", "tp"),
            P("sp", "tp"),
            P("sp", "tp"),
            P("sp", "tp"),
        ),
        check_vma=False,
    )
```
